32 devices in a mesh: grp: 2 (over y), sp: 4 (over z), tp: 4 (over x, core).
Axes of the slice: x: 2, y: 2, z: 4, core: 2. Of those that a mesh axis runs over, the one named last changes fastest.
Arguments:
- stream: bfloat16 [6144, 4096], P(('grp', 'sp'), 'tp'), parts along dimension 0, may hold values from -400 to 400
- in_weight: bfloat16 [2, 1024, 4096], P(None, 'sp', 'tp'), may hold values from -0.09375 to 0.09375
- out_weight: bfloat16 [2, 1024, 4096], P(None, 'sp', 'tp'), may hold values from -0.1875 to 0.1875
- group_mix: bfloat16 [2, 4, 256, 256], replicated, may hold values from -0.375 to 0.375
- pool_gain: float32 [2, 1024], replicated, may hold values from 0.1 to 1.9
- norm_gain: float32 [2, 4096], P(None, 'tp'), may hold values from 0.1 to 1.9
- norm_shift: float32 [2, 4096], P(None, 'tp'), may hold values from -3 to 3
Outputs:
- refined: bfloat16 [6144, 4096], P(('grp', 'sp'), 'tp'), parts along dimension 0
The draws below stay inside these ranges and needn't reach their ends.
There are 2 independent parts, one for each index of `grp`. The reference program is written for one: setup_inputs(seed, part) draws one part's arguments, and reference() takes and returns one part's arrays. A program takes and returns all parts, laid end to end along the dimension named above; an argument that names none is the same for every part. Nothing has to cross between parts.
All inputs are finite; a program needn't handle non-finite values.
Results may differ from the reference program's by a relative error of at most 0.015.
Values may be sent and summed in bfloat16 or wider, within the bound.
A program may use at most 64 MiB of HBM per device.

```python
import jax
import jax.numpy as jnp
from jax import lax

D = 4096
POOL = 1024
GROUPS = 4
GROUP_WIDTH = 256
LAYERS = 2
TOKENS = 3072
N_TP = 4


def draw_stream(key, part):
    base = jax.random.fold_in(key, 17)
    first_key, second_key = jax.random.split(base, 2)
    column = jnp.arange(D, dtype=jnp.float32) / D
    row_scale = 10.0 ** jax.random.uniform(second_key, (TOKENS, 1), jnp.float32)
    entries = jnp.clip(jax.random.normal(first_key, (TOKENS, D), jnp.float32), -4.0, 4.0)
    column_scale = 10.0 ** column
    return (entries * column_scale[None, :] * row_scale).astype(jnp.bfloat16)


def steps_of(rng, extent, cuts, smallest, high):
    factor_of, own = 1.0, jax.random.fold_in(rng, 6)
    for axis_at, shards_of in cuts:
        steps = jnp.exp(jax.random.uniform(jax.random.fold_in(own, axis_at), (shards_of,), jnp.float32, smallest / len(cuts), high / len(cuts)))
        factor_of = factor_of * jnp.repeat(steps, extent[axis_at] // shards_of).reshape([-1 if axis == axis_at else 1 for axis in range(len(extent))])
    return factor_of


def centred(stream_key, dims, scale, bound, cuts=(), kind=jnp.bfloat16):
    array = jax.random.normal(stream_key, dims, jnp.float32) * scale
    if len(cuts) > 0:
        array = steps_of(stream_key, dims, cuts, -0.22, 0.18) * array
    return jnp.clip(array, min=-bound, max=bound).astype(kind)


def setup_inputs(seed: int = 0, part: int = 0) -> dict:
    seeds = jax.random.split(jax.random.key(seed), 8)
    own_keys = jax.random.split(jax.random.fold_in(seeds[7], part), 8)
    return {
        "stream": draw_stream(jax.random.fold_in(jax.random.fold_in(seeds[7], part), 71), part),
        "in_weight": centred(seeds[1], (LAYERS, POOL, D), D ** -0.5, 0.09375, ((1, 4), (2, 4))),
        "out_weight": centred(seeds[2], (LAYERS, POOL, D), POOL ** -0.5, 0.1875, ((1, 4), (2, 4))),
        "group_mix": centred(seeds[3], (LAYERS, GROUPS, GROUP_WIDTH, GROUP_WIDTH), GROUP_WIDTH ** -0.5, 0.375),
        "pool_gain": jnp.clip(1.0 + 0.18 * jax.random.normal(seeds[4], (LAYERS, POOL), jnp.float32), 0.1, 1.9),
        "norm_gain": jnp.clip(1.0 + 0.18 * jax.random.normal(seeds[5], (LAYERS, D), jnp.float32), 0.1, 1.9),
        "norm_shift": centred(seeds[6], (LAYERS, D), 0.5, 3.0, ((1, 4),), jnp.float32),
    }


epsilon = 1e-05

def reference(stream, in_weight, out_weight, group_mix, pool_gain, norm_gain, norm_shift):
    tokens_total = stream.shape[0]
    channel_block = D // N_TP
    alpha = (2.0 * LAYERS) ** 0.25
    current = stream
    for layer_index in range(LAYERS):
        hidden_sum = jnp.zeros((tokens_total, POOL), jnp.float32)
        for part_index in range(N_TP):
            lower = part_index * channel_block
            upper = lower + channel_block
            term = jnp.dot(current[:, lower:upper], in_weight[layer_index][:, lower:upper].T, preferred_element_type=jnp.float32)
            rounded = lax.optimization_barrier(term.astype(jnp.bfloat16))
            hidden_sum = hidden_sum + rounded.astype(jnp.float32)
        hidden = hidden_sum.astype(jnp.bfloat16)
        positions = jnp.arange(1, tokens_total + 1, dtype=jnp.float32)[:, None]
        pooled_pieces = []
        for group_index in range(GROUPS):
            width = 2 ** (group_index + 1)
            group_cols = hidden[:, group_index * GROUP_WIDTH:(group_index + 1) * GROUP_WIDTH].astype(jnp.float32)
            padded = jnp.pad(group_cols, ((width - 1, 0), (0, 0)))
            window_sum = jnp.zeros_like(group_cols)
            for offset in range(width):
                window_sum = window_sum + padded[offset:offset + tokens_total]
            counts = jnp.minimum(positions, float(width))
            pooled_pieces.append(window_sum / counts - group_cols)
        pooled = jnp.concatenate(pooled_pieces, axis=1).astype(jnp.bfloat16)
        mixed_pieces = []
        for group_index in range(GROUPS):
            group_rows = pooled[:, group_index * GROUP_WIDTH:(group_index + 1) * GROUP_WIDTH]
            mixed_pieces.append(jnp.dot(group_rows, group_mix[layer_index, group_index], preferred_element_type=jnp.float32))
        scaled = (jnp.concatenate(mixed_pieces, axis=1) * pool_gain[layer_index][None, :]).astype(jnp.bfloat16)
        branch = jnp.dot(scaled, out_weight[layer_index], preferred_element_type=jnp.float32)
        summed = alpha * current.astype(jnp.float32) + branch
        row_mean = lax.optimization_barrier(jnp.sum(summed, axis=1)) / D
        row_var = lax.optimization_barrier(jnp.sum(summed * summed, axis=1)) / D - row_mean * row_mean
        normed = (summed - row_mean[:, None]) * lax.rsqrt(row_var + epsilon)[:, None]
        current = (normed * norm_gain[layer_index][None, :] + norm_shift[layer_index][None, :]).astype(jnp.bfloat16)
    return current
```

```python
import functools

import jax
import jax.numpy as jnp
from jax import lax
from jax.experimental import pallas as pl
from jax.experimental.pallas import tpu as pltpu
from jax.sharding import PartitionSpec as P

MESH = pl.DeviceIdType.MESH
EPSILON = 1e-05
F32 = jnp.float32
BF16 = jnp.bfloat16
REACH = 16
NT = (((1,), (1,)), ((), ()))


def arrival_orders(n):
    orders = []
    for z in range(n):
        first = 1 if z < n / 2 else -1
        order = [z]
        for d in range(1, n):
            order += [b for b in (z + first * d, z - first * d) if 0 <= b < n]
        orders.append(order)
    return orders


def kernel(cfg, *refs):
    n, tp_n, layers, groups, width, streamed = cfg
    (stream, w_in, w_out, mix, gain, norm_gain, norm_shift, out,
     wg, cur, acc, psend, precv, pown, xsend, xrecv, hbuf, hsend, hrecv, sc, tsend, trecv,
     loc_sem, own_send, f_send, z_recv, y_send, y_recv,
     p_send_s, p_recv_s, x_send_s, x_recv_s, h_send_s, h_recv_s,
     c_send_s, c_recv_s, t_send_s, t_recv_s, out_sem) = refs
    tokens, chans = cur.shape
    half = tokens // 2
    block = 256
    chunks = tokens // block
    d_model = chans * tp_n
    alpha = (2.0 * layers) ** 0.25
    nx = tp_n // 2
    y, z, t = lax.axis_index("grp"), lax.axis_index("sp"), lax.axis_index("tp")
    core, x = lax.rem(t, 2), t // 2
    sib = t + 1 - 2 * core
    orders = arrival_orders(n)
    mine, other = core * half, (1 - core) * half
    mine = pl.multiple_of(mine, half)
    other = pl.multiple_of(other, half)

    def order(s):
        if not streamed:
            return jnp.int32(s)
        b = jnp.int32(0)
        for k in range(n):
            b = jnp.where(z == k, orders[k][s], b)
        return b

    def remote(src, dst, ssem, rsem, device):
        return pltpu.make_async_remote_copy(
            src_ref=src, dst_ref=dst, send_sem=ssem, recv_sem=rsem,
            device_id=device, device_id_type=MESH)

    rows = w_in.shape[1]
    copies = [pltpu.make_async_copy(stream, cur, loc_sem.at[0])]
    for m in range(2 * layers):
        src = (w_in, w_out)[m % 2].at[m // 2]
        if streamed:
            dst = wg.at[m, pl.ds(pl.multiple_of(z * rows, rows), rows)]
        else:
            dst = wg.at[m]
        copies.append(pltpu.make_async_copy(src, dst, loc_sem.at[1 + m]))
    for copy in copies:
        copy.start()

    barrier = pltpu.get_barrier_semaphore()

    def greet(device):
        pl.semaphore_signal(barrier, inc=1, device_id=device, device_id_type=MESH)

    for k in range(1, tp_n):
        greet((y, z, lax.rem(t + k, tp_n)))
    count = jnp.int32(tp_n - 1)
    if streamed:
        greet((1 - y, z, t))
        count = count + 1

        @pl.when(z > 0)
        def _():
            greet((y, z - 1, t))

        @pl.when(z < n - 1)
        def _():
            greet((y, z + 1, t))

        count = count + jnp.where(z > 0, 1, 0) + jnp.where(z < n - 1, 1, 0)
    down = (core == 1) & (z < n - 1)
    up = (core == 0) & (z > 0)

    @pl.when(down)
    def _():
        greet((y, z + 1, sib))

    @pl.when(up)
    def _():
        greet((y, z - 1, sib))

    count = count + jnp.where(down, 1, 0) + jnp.where(up, 1, 0)
    pl.semaphore_wait(barrier, count)

    part = rows // 2

    def own_copy(m, side):
        src = (w_in, w_out)[m % 2].at[m // 2, pl.ds(pl.multiple_of(y * part, part), part)]
        dst = wg.at[m, pl.ds(pl.multiple_of(z * rows + y * part, part), part)]
        return remote(src, dst, own_send.at[m, side], z_recv.at[m, z], (y, z + 2 * side - 1, t))

    def own_each(m, what):
        for side in (1, 0):
            @pl.when(z < n - 1 if side else z > 0)
            def _(side=side):
                what(own_copy(m, side))

    def piece(m, b, from_y):
        return wg.at[m, pl.ds(pl.multiple_of(b * rows + from_y * part, part), part)]

    def onward(m, b):
        zt = jnp.where(b < z, z + 1, z - 1)
        ref = piece(m, b, y)
        return (zt >= 0) & (zt < n), remote(ref, ref, f_send.at[m, b], z_recv.at[m, b], (y, zt, t))

    def across(m, b, from_y):
        ref = piece(m, b, from_y)
        return remote(ref, ref, y_send.at[m, b], y_recv.at[m, b], (1 - y, z, t))

    events = [(m, s) for m in range(2 * layers) for s in range(1, n)]
    state = [0]

    def advance(m, s, ahead=0):
        if not streamed:
            return
        goal = min(m * (n - 1) + s + ahead, len(events))
        while state[0] < goal:
            em, es = events[state[0]]
            state[0] += 1
            b = order(es)
            there, copy = onward(em, b)
            copy.wait_recv()
            pl.when(there)(copy.start)
            across(em, b, y).start()
            if es == 2 and em + 2 < 2 * layers:
                own_each(em + 2, lambda c: c.start())

    def ready(m, s):
        if s == 0 or not streamed:
            if s == 0:
                copies[1 + m].wait()
        else:
            across(m, order(s), 1 - y).wait_recv()

    def weight(m, s):
        return wg[m, pl.ds(pl.multiple_of(order(s) * block, block), block), :]

    def p_copy(l, s):
        return remote(psend.at[l, s], precv.at[l, s], p_send_s.at[l, s], p_recv_s.at[l, s], (y, z, sib))

    def x_copies(l, s):
        return [remote(xsend.at[l, s], xrecv.at[k - 1, l, s], x_send_s.at[k - 1, l, s],
                       x_recv_s.at[k - 1, l, s], (y, z, lax.rem(x + k, nx) * 2 + core))
                for k in range(1, nx)]

    def h_copy(l, s):
        b = order(s)
        return remote(hsend.at[l, b], hrecv.at[l, b], h_send_s.at[l, b], h_recv_s.at[l, b],
                      (y, z + core, sib))

    def c_copy(l, s, at):
        ref = sc.at[l, s, pl.ds(at, half)]
        return remote(ref, ref, c_send_s.at[l, s], c_recv_s.at[l, s], (y, z, sib))

    def t_copies(l, i):
        return [remote(tsend.at[l, i], trecv.at[k - 1, l, i], t_send_s.at[k - 1, l, i],
                       t_recv_s.at[k - 1, l, i], (y, z, lax.rem(t + k, tp_n)))
                for k in range(1, tp_n)]

    h_out = (core == 0) | (z < n - 1)
    h_in = (core == 1) | (z > 0)

    def project(l, s):
        w = weight(2 * l, s)
        psend[l, s] = lax.dot_general(
            cur[pl.ds(other, half), :], w, NT, preferred_element_type=F32).astype(BF16)
        p_copy(l, s).start()
        pown[s] = lax.dot_general(cur[pl.ds(mine, half), :], w, NT, preferred_element_type=F32)

    def chip_sum(l, s):
        p_copy(l, s).wait_recv()
        total = pown[s] + precv[l, s].astype(F32)
        pown[s] = total
        xsend[l, s] = total.astype(BF16)
        for copy in x_copies(l, s):
            copy.start()

    def finish_hidden(l, s):
        total = pown[s]
        for k, copy in enumerate(x_copies(l, s)):
            copy.wait_recv()
            total = total + xrecv[k, l, s].astype(F32)
        hidden = total.astype(BF16)
        hbuf[s, REACH:, :] = hidden.astype(F32)
        hsend[l, order(s)] = hidden[half - REACH:, :]
        pl.when(h_out)(h_copy(l, s).start)

    def pool(l, s):
        b = order(s)

        @pl.when(h_in)
        def _():
            h_copy(l, s).wait_recv()
            hbuf[s, :REACH, :] = hrecv[l, b].astype(F32)

        @pl.when(jnp.logical_not(h_in))
        def _():
            hbuf[s, :REACH, :] = jnp.zeros((REACH, width), F32)

        ext = hbuf[s]
        run = ext + pltpu.roll(ext, 1, 0)
        for octave in range(1, groups):
            take = jnp.where(b >= octave, 1.0, 0.0).astype(F32)
            run = run + take * pltpu.roll(run, 2**octave, 0)
        reach = jnp.int32(2)
        for octave in range(1, groups):
            reach = jnp.where(b >= octave, 2 ** (octave + 1), reach)
        at = z * tokens + core * half + 1 + lax.broadcasted_iota(jnp.int32, (half, width), 0)
        counts = jnp.minimum(at, reach).astype(F32)
        pooled = (run[REACH:, :] / counts - ext[REACH:, :]).astype(BF16)
        mixed = jnp.dot(pooled, mix[l, b], preferred_element_type=F32)
        sc[l, s, pl.ds(mine, half), :] = (mixed * gain[l, b]).astype(BF16)
        c_copy(l, s, mine).start()

    def expand(l, s):
        c_copy(l, s, other).wait_recv()
        at_m = 2 * l + 1

        def body(i, carry):
            r = pl.ds(pl.multiple_of(i * block, block), block)
            add = jnp.dot(sc[l, s, r, :], weight(at_m, s), preferred_element_type=F32)
            if s == 0:
                acc[r, :] = alpha * cur[r, :].astype(F32) + add
            else:
                acc[r, :] = acc[r, :] + add
            return carry

        if s < groups - 1:
            lax.fori_loop(0, chunks, body, 0)
            return
        for i in range(chunks):
            body(i, 0)
            v = acc[i * block:(i + 1) * block, :]
            lane = lax.broadcasted_iota(jnp.int32, (block, 128), 1)
            row_sum = jnp.sum(v, axis=1, keepdims=True)
            row_squares = jnp.sum(v * v, axis=1, keepdims=True)
            both = jnp.where(lane == 0, row_sum, jnp.where(lane == 1, row_squares, 0.0))
            tsend[l, i] = both.T[:8, :]
            for copy in t_copies(l, i):
                copy.start()

    def norm(l):
        dst = out if l == layers - 1 else cur
        for i in range(chunks):
            stats = tsend[l, i]
            for k, copy in enumerate(t_copies(l, i)):
                copy.wait_recv()
                stats = stats + trecv[k, l, i]
            stats = stats / d_model
            mean = stats[0:1, :]
            var = stats[1:2, :] - mean * mean
            inv = lax.rsqrt(var + EPSILON)
            row = lax.broadcasted_iota(jnp.int32, (128, block), 0)
            cols = jnp.where(row == 0, mean, jnp.where(row == 1, inv, 0.0)).T
            r = slice(i * block, (i + 1) * block)
            v = (acc[r, :] - cols[:, 0:1]) * cols[:, 1:2]
            dst[r, :] = (v * norm_gain[l:l + 1, :] + norm_shift[l:l + 1, :]).astype(BF16)

    if streamed:
        own_each(0, lambda c: c.start())
        own_each(1, lambda c: c.start())
    copies[0].wait()
    last = groups - 1
    for l in range(layers):
        mi, mo = 2 * l, 2 * l + 1
        ready(mi, 0)
        project(l, 0)
        for s in range(1, groups):
            advance(mi, s, 1)
            chip_sum(l, s - 1)
            ready(mi, s)
            project(l, s)
        chip_sum(l, last)
        for s in range(groups):
            finish_hidden(l, s)
        advance(mo, 2)
        for s in range(groups):
            pool(l, s)
        ready(mo, 0)
        expand(l, 0)
        for s in range(1, groups):
            advance(mo, s, 1)
            ready(mo, s)
            expand(l, s)
        norm(l)

    if streamed:
        for m in range(2 * layers):
            own_each(m, lambda c: c.wait_send())
            for s in range(1, n):
                b = order(s)
                there, copy = onward(m, b)
                pl.when(there)(copy.wait_send)
                across(m, b, y).wait_send()
    for l in range(layers):
        for s in range(groups):
            p_copy(l, s).wait_send()
            for copy in x_copies(l, s):
                copy.wait_send()
            pl.when(h_out)(h_copy(l, s).wait_send)
            c_copy(l, s, mine).wait_send()
        for i in range(chunks):
            for copy in t_copies(l, i):
                copy.wait_send()


def per_device(n, grp_n, tp_n, stream, in_weight, out_weight, group_mix, pool_gain, norm_gain, norm_shift):
    layers, groups, width = group_mix.shape[:3]
    tokens, chans = stream.shape
    pool = groups * width
    streamed = n == groups and grp_n == 2
    if not streamed:
        in_weight = lax.all_gather(in_weight, "sp", axis=1, tiled=True)
        out_weight = lax.all_gather(out_weight, "sp", axis=1, tiled=True)
    nx = tp_n // 2
    half = tokens // 2
    chunks = tokens // 256
    ms = 2 * layers
    dma = pltpu.SemaphoreType.DMA
    any_spec = pl.BlockSpec(memory_space=pl.ANY)
    vmem = pl.BlockSpec(memory_space=pltpu.VMEM)
    xs = max(nx - 1, 1)
    return pl.pallas_call(
        functools.partial(kernel, (n, tp_n, layers, groups, width, streamed)),
        out_shape=jax.ShapeDtypeStruct((tokens, chans), BF16),
        in_specs=[any_spec] * 3 + [vmem] * 4,
        out_specs=vmem,
        scratch_shapes=[
            pltpu.VMEM((ms, pool, chans), BF16),
            pltpu.VMEM((tokens, chans), BF16),
            pltpu.VMEM((tokens, chans), F32),
            pltpu.VMEM((layers, groups, half, width), BF16),
            pltpu.VMEM((layers, groups, half, width), BF16),
            pltpu.VMEM((groups, half, width), F32),
            pltpu.VMEM((layers, groups, half, width), BF16),
            pltpu.VMEM((xs, layers, groups, half, width), BF16),
            pltpu.VMEM((groups, REACH + half, width), F32),
            pltpu.VMEM((layers, groups, REACH, width), BF16),
            pltpu.VMEM((layers, groups, REACH, width), BF16),
            pltpu.VMEM((layers, groups, tokens, width), BF16),
            pltpu.VMEM((layers, chunks, 8, 256), F32),
            pltpu.VMEM((tp_n - 1, layers, chunks, 8, 256), F32),
            dma((1 + ms,)),
            dma((ms, 2)), dma((ms, groups)), dma((ms, groups)), dma((ms, groups)), dma((ms, groups)),
            dma((layers, groups)), dma((layers, groups)),
            dma((xs, layers, groups)), dma((xs, layers, groups)),
            dma((layers, groups)), dma((layers, groups)),
            dma((layers, groups)), dma((layers, groups)),
            dma((tp_n - 1, layers, chunks)), dma((tp_n - 1, layers, chunks)),
            dma((1,)),
        ],
        compiler_params=pltpu.CompilerParams(
            collective_id=0, has_side_effects=True, vmem_limit_bytes=56 * 1024 * 1024),
    )(stream, in_weight, out_weight, group_mix,
      pool_gain.reshape(layers, groups, 1, width), norm_gain, norm_shift)


def solution(mesh):
    in_specs = (
        P(("grp", "sp"), "tp"),
        P(None, "sp", "tp"),
        P(None, "sp", "tp"),
        P(),
        P(),
        P(None, "tp"),
        P(None, "tp"),
    )
    out_specs = P(("grp", "sp"), "tp")
    sizes = mesh.shape
    body = functools.partial(per_device, sizes["sp"], sizes["grp"], sizes["tp"])
    return jax.shard_map(
        body, mesh=mesh, in_specs=in_specs, out_specs=out_specs, check_vma=False
    )
```

```python
import functools

import jax
import jax.numpy as jnp
from jax import lax
from jax.experimental import pallas as pl
from jax.experimental.pallas import tpu as pltpu
from jax.sharding import PartitionSpec as P

MESH = pl.DeviceIdType.MESH
EPSILON = 1e-05
F32 = jnp.float32
BF16 = jnp.bfloat16
REACH = 16
PIECES = 2
NT = (((1,), (1,)), ((), ()))


def arrival_orders(n):
    orders = []
    for z in range(n):
        first = 1 if z < n / 2 else -1
        order = [z]
        for d in range(1, n):
            order += [b for b in (z + first * d, z - first * d) if 0 <= b < n]
        orders.append(order)
    return orders


def kernel(cfg, *refs):
    n, tp_n, layers, groups, width, streamed = cfg
    (stream, w_in, w_out, mix, gain, norm_gain, norm_shift, out,
     wg, cur, acc, psend, precv, pown, xsend, xrecv, hbuf, hsend, hrecv, sc, tsend, trecv,
     loc_sem, own_send, f_send, z_recv, y_send, y_recv,
     p_send_s, p_recv_s, x_send_s, x_recv_s, h_send_s, h_recv_s,
     c_send_s, c_recv_s, t_send_s, t_recv_s, out_sem) = refs
    tokens, chans = cur.shape
    half = tokens // 2
    block = 256
    chunks = tokens // block
    d_model = chans * tp_n
    alpha = (2.0 * layers) ** 0.25
    nx = tp_n // 2
    y, z, t = lax.axis_index("grp"), lax.axis_index("sp"), lax.axis_index("tp")
    core, x = lax.rem(t, 2), t // 2
    sib = t + 1 - 2 * core
    orders = arrival_orders(n)
    mine, other = core * half, (1 - core) * half
    mine = pl.multiple_of(mine, half)
    other = pl.multiple_of(other, half)

    def order(s):
        if not streamed:
            return jnp.int32(s)
        b = jnp.int32(0)
        for k in range(n):
            b = jnp.where(z == k, orders[k][s], b)
        return b

    def remote(src, dst, ssem, rsem, device):
        return pltpu.make_async_remote_copy(
            src_ref=src, dst_ref=dst, send_sem=ssem, recv_sem=rsem,
            device_id=device, device_id_type=MESH)

    rows = w_in.shape[1]
    copies = [pltpu.make_async_copy(stream, cur, loc_sem.at[0])]
    for m in range(2 * layers):
        src = (w_in, w_out)[m % 2].at[m // 2]
        if streamed:
            dst = wg.at[m, pl.ds(pl.multiple_of(z * rows, rows), rows)]
        else:
            dst = wg.at[m]
        copies.append(pltpu.make_async_copy(src, dst, loc_sem.at[1 + m]))
    for copy in copies:
        copy.start()

    barrier = pltpu.get_barrier_semaphore()

    def greet(device):
        pl.semaphore_signal(barrier, inc=1, device_id=device, device_id_type=MESH)

    for k in range(1, tp_n):
        greet((y, z, lax.rem(t + k, tp_n)))
    count = jnp.int32(tp_n - 1)
    if streamed:
        greet((1 - y, z, t))
        count = count + 1

        @pl.when(z > 0)
        def _():
            greet((y, z - 1, t))

        @pl.when(z < n - 1)
        def _():
            greet((y, z + 1, t))

        count = count + jnp.where(z > 0, 1, 0) + jnp.where(z < n - 1, 1, 0)
    down = (core == 1) & (z < n - 1)
    up = (core == 0) & (z > 0)

    @pl.when(down)
    def _():
        greet((y, z + 1, sib))

    @pl.when(up)
    def _():
        greet((y, z - 1, sib))

    count = count + jnp.where(down, 1, 0) + jnp.where(up, 1, 0)
    pl.semaphore_wait(barrier, count)

    part = rows // 2
    cut = part // PIECES

    def span(base, q):
        return pl.ds(pl.multiple_of(base + q * cut, cut), cut)

    def own_copy(m, side, q):
        src = (w_in, w_out)[m % 2].at[m // 2, span(y * part, q)]
        dst = wg.at[m, span(z * rows + y * part, q)]
        return remote(src, dst, own_send.at[m, side, q], z_recv.at[m, z, q], (y, z + 2 * side - 1, t))

    def own_side(m, side, when, what):
        @pl.when(when & (z < n - 1 if side else z > 0))
        def _():
            for q in range(PIECES):
                what(own_copy(m, side, q))

    def onward(m, b, q):
        zt = jnp.where(b < z, z + 1, z - 1)
        ref = wg.at[m, span(b * rows + y * part, q)]
        return (zt >= 0) & (zt < n), remote(
            ref, ref, f_send.at[m, b, q], z_recv.at[m, b, q], (y, zt, t))

    def across(m, b, from_y, q):
        ref = wg.at[m, span(b * rows + from_y * part, q)]
        return remote(ref, ref, y_send.at[m, b, q], y_recv.at[m, b, q], (1 - y, z, t))

    events = [(m, s, q) for m in range(2 * layers) for s in range(1, n) for q in range(PIECES)]
    state = [0]

    def forwards_end(k, side):
        steps = [s for s in range(1, n) if (orders[k][s] < k if side else orders[k][s] > k)]
        return max(steps, default=0)

    def advance(m, s, ahead=0):
        if not streamed:
            return
        goal = min((m * (n - 1) + s) * PIECES + ahead, len(events))
        while state[0] < goal:
            em, es, q = events[state[0]]
            state[0] += 1
            b = order(es)
            there, copy = onward(em, b, q)
            copy.wait_recv()
            pl.when(there)(copy.start)
            across(em, b, y, q).start()
            if q == PIECES - 1 and em + 1 < 2 * layers:
                for side in (1, 0):
                    places = [k for k in range(n) if forwards_end(k, side) == es]
                    for k in places:
                        own_side(em + 1, side, z == k, lambda c: c.start())

    def ready(m, s):
        if s == 0:
            copies[1 + m].wait()
        elif streamed:
            for q in range(PIECES):
                across(m, order(s), 1 - y, q).wait_recv()

    def weight(m, s):
        return wg[m, pl.ds(pl.multiple_of(order(s) * block, block), block), :]

    def p_copy(l, s):
        return remote(psend.at[l, s], precv.at[l, s], p_send_s.at[l, s], p_recv_s.at[l, s], (y, z, sib))

    def x_copies(l, s):
        return [remote(xsend.at[l, s], xrecv.at[k - 1, l, s], x_send_s.at[k - 1, l, s],
                       x_recv_s.at[k - 1, l, s], (y, z, lax.rem(x + k, nx) * 2 + core))
                for k in range(1, nx)]

    def h_copy(l, s):
        b = order(s)
        return remote(hsend.at[l, b], hrecv.at[l, b], h_send_s.at[l, b], h_recv_s.at[l, b],
                      (y, z + core, sib))

    def c_copy(l, s, at):
        ref = sc.at[l, s, pl.ds(at, half)]
        return remote(ref, ref, c_send_s.at[l, s], c_recv_s.at[l, s], (y, z, sib))

    def t_copies(l, i):
        return [remote(tsend.at[l, i], trecv.at[k - 1, l, i], t_send_s.at[k - 1, l, i],
                       t_recv_s.at[k - 1, l, i], (y, z, lax.rem(t + k, tp_n)))
                for k in range(1, tp_n)]

    h_out = (core == 0) | (z < n - 1)
    h_in = (core == 1) | (z > 0)

    def project(l, s):
        w = weight(2 * l, s)
        psend[l, s] = lax.dot_general(
            cur[pl.ds(other, half), :], w, NT, preferred_element_type=F32).astype(BF16)
        p_copy(l, s).start()
        pown[s] = lax.dot_general(cur[pl.ds(mine, half), :], w, NT, preferred_element_type=F32)

    def chip_sum(l, s):
        p_copy(l, s).wait_recv()
        total = pown[s] + precv[l, s].astype(F32)
        pown[s] = total
        xsend[l, s] = total.astype(BF16)
        for copy in x_copies(l, s):
            copy.start()

    def finish_hidden(l, s):
        total = pown[s]
        for k, copy in enumerate(x_copies(l, s)):
            copy.wait_recv()
            total = total + xrecv[k, l, s].astype(F32)
        hidden = total.astype(BF16)
        hbuf[s, REACH:, :] = hidden.astype(F32)
        hsend[l, order(s)] = hidden[half - REACH:, :]
        pl.when(h_out)(h_copy(l, s).start)

    def pool(l, s):
        b = order(s)

        @pl.when(h_in)
        def _():
            h_copy(l, s).wait_recv()
            hbuf[s, :REACH, :] = hrecv[l, b].astype(F32)

        @pl.when(jnp.logical_not(h_in))
        def _():
            hbuf[s, :REACH, :] = jnp.zeros((REACH, width), F32)

        ext = hbuf[s]
        run = ext + pltpu.roll(ext, 1, 0)
        for octave in range(1, groups):
            take = jnp.where(b >= octave, 1.0, 0.0).astype(F32)
            run = run + take * pltpu.roll(run, 2**octave, 0)
        reach = jnp.int32(2)
        for octave in range(1, groups):
            reach = jnp.where(b >= octave, 2 ** (octave + 1), reach)
        at = z * tokens + core * half + 1 + lax.broadcasted_iota(jnp.int32, (half, width), 0)
        counts = jnp.minimum(at, reach).astype(F32)
        pooled = (run[REACH:, :] / counts - ext[REACH:, :]).astype(BF16)
        mixed = jnp.dot(pooled, mix[l, b], preferred_element_type=F32)
        sc[l, s, pl.ds(mine, half), :] = (mixed * gain[l:l + 1, pl.ds(pl.multiple_of(b * width, width), width)]).astype(BF16)
        c_copy(l, s, mine).start()

    def expand(l, s):
        c_copy(l, s, other).wait_recv()
        at_m = 2 * l + 1

        def body(i, carry):
            r = pl.ds(pl.multiple_of(i * block, block), block)
            add = jnp.dot(sc[l, s, r, :], weight(at_m, s), preferred_element_type=F32)
            if s == 0:
                acc[r, :] = alpha * cur[r, :].astype(F32) + add
            else:
                acc[r, :] = acc[r, :] + add
            return carry

        if s < groups - 1:
            lax.fori_loop(0, chunks, body, 0)
            return
        for i in range(chunks):
            body(i, 0)
            v = acc[i * block:(i + 1) * block, :]
            lane = lax.broadcasted_iota(jnp.int32, (block, 128), 1)
            row_sum = jnp.sum(v, axis=1, keepdims=True)
            row_squares = jnp.sum(v * v, axis=1, keepdims=True)
            both = jnp.where(lane == 0, row_sum, jnp.where(lane == 1, row_squares, 0.0))
            tsend[l, i] = both.T[:8, :]
            for copy in t_copies(l, i):
                copy.start()

    def norm(l):
        dst = out if l == layers - 1 else cur
        for i in range(chunks):
            stats = tsend[l, i]
            for k, copy in enumerate(t_copies(l, i)):
                copy.wait_recv()
                stats = stats + trecv[k, l, i]
            stats = stats / d_model
            mean = stats[0:1, :]
            var = stats[1:2, :] - mean * mean
            inv = lax.rsqrt(var + EPSILON)
            row = lax.broadcasted_iota(jnp.int32, (128, block), 0)
            cols = jnp.where(row == 0, mean, jnp.where(row == 1, inv, 0.0)).T
            r = slice(i * block, (i + 1) * block)
            v = (acc[r, :] - cols[:, 0:1]) * cols[:, 1:2]
            dst[r, :] = (v * norm_gain[l:l + 1, :] + norm_shift[l:l + 1, :]).astype(BF16)

    if streamed:
        for m in range(2 * layers):
            for side in (1, 0):
                first = (z >= 0) if m == 0 else (z == 0 if side else z == n - 1)
                own_side(m, side, first, lambda c: c.start())
    copies[0].wait()
    last = groups - 1
    for l in range(layers):
        mi, mo = 2 * l, 2 * l + 1
        ready(mi, 0)
        project(l, 0)
        for s in range(1, groups):
            advance(mi, s, 2)
            chip_sum(l, s - 1)
            ready(mi, s)
            project(l, s)
        chip_sum(l, last)
        for s in range(groups):
            finish_hidden(l, s)
        pool(l, 0)
        pool(l, 1)
        advance(mo, 2)
        for s in range(2, groups):
            pool(l, s)
        ready(mo, 0)
        expand(l, 0)
        for s in range(1, groups):
            advance(mo, s, 2)
            ready(mo, s)
            expand(l, s)
        norm(l)

    if streamed:
        for m in range(2 * layers):
            for side in (1, 0):
                own_side(m, side, z >= 0, lambda c: c.wait_send())
            for s in range(1, n):
                b = order(s)
                for q in range(PIECES):
                    there, copy = onward(m, b, q)
                    pl.when(there)(copy.wait_send)
                    across(m, b, y, q).wait_send()
    for l in range(layers):
        for s in range(groups):
            p_copy(l, s).wait_send()
            for copy in x_copies(l, s):
                copy.wait_send()
            pl.when(h_out)(h_copy(l, s).wait_send)
            c_copy(l, s, mine).wait_send()
        for i in range(chunks):
            for copy in t_copies(l, i):
                copy.wait_send()


def per_device(n, grp_n, tp_n, stream, in_weight, out_weight, group_mix, pool_gain, norm_gain, norm_shift):
    layers, groups, width = group_mix.shape[:3]
    tokens, chans = stream.shape
    pool = groups * width
    streamed = n == groups and grp_n == 2
    if not streamed:
        in_weight = lax.all_gather(in_weight, "sp", axis=1, tiled=True)
        out_weight = lax.all_gather(out_weight, "sp", axis=1, tiled=True)
    nx = tp_n // 2
    half = tokens // 2
    chunks = tokens // 256
    ms = 2 * layers
    dma = pltpu.SemaphoreType.DMA
    any_spec = pl.BlockSpec(memory_space=pl.ANY)
    vmem = pl.BlockSpec(memory_space=pltpu.VMEM)
    xs = max(nx - 1, 1)
    return pl.pallas_call(
        functools.partial(kernel, (n, tp_n, layers, groups, width, streamed)),
        out_shape=jax.ShapeDtypeStruct((tokens, chans), BF16),
        in_specs=[any_spec] * 3 + [vmem] * 4,
        out_specs=vmem,
        scratch_shapes=[
            pltpu.VMEM((ms, pool, chans), BF16),
            pltpu.VMEM((tokens, chans), BF16),
            pltpu.VMEM((tokens, chans), F32),
            pltpu.VMEM((layers, groups, half, width), BF16),
            pltpu.VMEM((layers, groups, half, width), BF16),
            pltpu.VMEM((groups, half, width), F32),
            pltpu.VMEM((layers, groups, half, width), BF16),
            pltpu.VMEM((xs, layers, groups, half, width), BF16),
            pltpu.VMEM((groups, REACH + half, width), F32),
            pltpu.VMEM((layers, groups, REACH, width), BF16),
            pltpu.VMEM((layers, groups, REACH, width), BF16),
            pltpu.VMEM((layers, groups, tokens, width), BF16),
            pltpu.VMEM((layers, chunks, 8, 256), F32),
            pltpu.VMEM((tp_n - 1, layers, chunks, 8, 256), F32),
            dma((1 + ms,)),
            dma((ms, 2, PIECES)), dma((ms, groups, PIECES)), dma((ms, groups, PIECES)),
            dma((ms, groups, PIECES)), dma((ms, groups, PIECES)),
            dma((layers, groups)), dma((layers, groups)),
            dma((xs, layers, groups)), dma((xs, layers, groups)),
            dma((layers, groups)), dma((layers, groups)),
            dma((layers, groups)), dma((layers, groups)),
            dma((tp_n - 1, layers, chunks)), dma((tp_n - 1, layers, chunks)),
            dma((1,)),
        ],
        compiler_params=pltpu.CompilerParams(
            collective_id=0, has_side_effects=True, vmem_limit_bytes=56 * 1024 * 1024),
    )(stream, in_weight, out_weight, group_mix,
      pool_gain, norm_gain, norm_shift)


def solution(mesh):
    in_specs = (
        P(("grp", "sp"), "tp"),
        P(None, "sp", "tp"),
        P(None, "sp", "tp"),
        P(),
        P(),
        P(None, "tp"),
        P(None, "tp"),
    )
    out_specs = P(("grp", "sp"), "tp")
    sizes = mesh.shape
    body = functools.partial(per_device, sizes["sp"], sizes["grp"], sizes["tp"])
    return jax.shard_map(
        body, mesh=mesh, in_specs=in_specs, out_specs=out_specs, check_vma=False
    )
```

```python
import functools

import jax
import jax.numpy as jnp
from jax import lax
from jax.experimental import pallas as pl
from jax.experimental.pallas import tpu as pltpu
from jax.sharding import PartitionSpec as P

MESH = pl.DeviceIdType.MESH
EPSILON = 1e-05
F32 = jnp.float32
BF16 = jnp.bfloat16
REACH = 16
PIECES = 2
NT = (((1,), (1,)), ((), ()))


def arrival_orders(n):
    orders = []
    for z in range(n):
        first = 1 if z < n / 2 else -1
        order = [z]
        for d in range(1, n):
            order += [b for b in (z + first * d, z - first * d) if 0 <= b < n]
        orders.append(order)
    return orders


def kernel(cfg, *refs):
    n, tp_n, layers, groups, width, streamed = cfg
    (stream, w_in, w_out, mix, gain, norm_gain, norm_shift, out,
     wg, cur, acc, psend, precv, pown, xsend, xrecv, hbuf, hsend, hrecv, sc, tsend, trecv,
     loc_sem, own_send, f_send, z_recv, y_send, y_recv,
     p_send_s, p_recv_s, x_send_s, x_recv_s, h_send_s, h_recv_s,
     c_send_s, c_recv_s, t_send_s, t_recv_s, out_sem) = refs
    tokens, chans = cur.shape
    half = tokens // 2
    block = 256
    chunks = tokens // block
    d_model = chans * tp_n
    alpha = (2.0 * layers) ** 0.25
    nx = tp_n // 2
    y, z, t = lax.axis_index("grp"), lax.axis_index("sp"), lax.axis_index("tp")
    core, x = lax.rem(t, 2), t // 2
    sib = t + 1 - 2 * core
    orders = arrival_orders(n)
    mine, other = core * half, (1 - core) * half
    mine = pl.multiple_of(mine, half)
    other = pl.multiple_of(other, half)

    def order(s):
        if not streamed:
            return jnp.int32(s)
        b = jnp.int32(0)
        for k in range(n):
            b = jnp.where(z == k, orders[k][s], b)
        return b

    def remote(src, dst, ssem, rsem, device):
        return pltpu.make_async_remote_copy(
            src_ref=src, dst_ref=dst, send_sem=ssem, recv_sem=rsem,
            device_id=device, device_id_type=MESH)

    rows = w_in.shape[1]
    copies = [pltpu.make_async_copy(stream, cur, loc_sem.at[0])]
    for m in range(2 * layers):
        src = (w_in, w_out)[m % 2].at[m // 2]
        if streamed:
            dst = wg.at[m, pl.ds(pl.multiple_of(z * rows, rows), rows)]
        else:
            dst = wg.at[m]
        copies.append(pltpu.make_async_copy(src, dst, loc_sem.at[1 + m]))
    for copy in copies:
        copy.start()

    barrier = pltpu.get_barrier_semaphore()

    def greet(device):
        pl.semaphore_signal(barrier, inc=1, device_id=device, device_id_type=MESH)

    for k in range(1, tp_n):
        greet((y, z, lax.rem(t + k, tp_n)))
    count = jnp.int32(tp_n - 1)
    if streamed:
        greet((1 - y, z, t))
        count = count + 1

        @pl.when(z > 0)
        def _():
            greet((y, z - 1, t))

        @pl.when(z < n - 1)
        def _():
            greet((y, z + 1, t))

        count = count + jnp.where(z > 0, 1, 0) + jnp.where(z < n - 1, 1, 0)
    down = (core == 1) & (z < n - 1)
    up = (core == 0) & (z > 0)

    @pl.when(down)
    def _():
        greet((y, z + 1, sib))

    @pl.when(up)
    def _():
        greet((y, z - 1, sib))

    count = count + jnp.where(down, 1, 0) + jnp.where(up, 1, 0)
    pl.semaphore_wait(barrier, count)

    part = rows // 2
    cut = part // PIECES

    def span(base, q):
        return pl.ds(pl.multiple_of(base + q * cut, cut), cut)

    def own_copy(m, side, q):
        src = (w_in, w_out)[m % 2].at[m // 2, span(y * part, q)]
        dst = wg.at[m, span(z * rows + y * part, q)]
        return remote(src, dst, own_send.at[m, side, q], z_recv.at[m, z, q], (y, z + 2 * side - 1, t))

    def own_side(m, side, when, what):
        @pl.when(when & (z < n - 1 if side else z > 0))
        def _():
            for q in range(PIECES):
                what(own_copy(m, side, q))

    def onward(m, b, q):
        zt = jnp.where(b < z, z + 1, z - 1)
        ref = wg.at[m, span(b * rows + y * part, q)]
        return (zt >= 0) & (zt < n), remote(
            ref, ref, f_send.at[m, b, q], z_recv.at[m, b, q], (y, zt, t))

    def across(m, b, from_y, q):
        ref = wg.at[m, span(b * rows + from_y * part, q)]
        return remote(ref, ref, y_send.at[m, b, q], y_recv.at[m, b, q], (1 - y, z, t))

    events = [(m, s, q) for m in range(2 * layers) for s in range(1, n) for q in range(PIECES)]
    state = [0]

    def forwards_end(k, side):
        steps = [s for s in range(1, n) if (orders[k][s] < k if side else orders[k][s] > k)]
        return max(steps, default=0)

    def advance(m, s, ahead=0):
        if not streamed:
            return
        goal = min((m * (n - 1) + s) * PIECES + ahead, len(events))
        while state[0] < goal:
            em, es, q = events[state[0]]
            state[0] += 1
            b = order(es)
            there, copy = onward(em, b, q)
            copy.wait_recv()
            pl.when(there)(copy.start)
            across(em, b, y, q).start()
            if q == PIECES - 1 and em + 1 < 2 * layers:
                for side in (1, 0):
                    places = [k for k in range(n) if forwards_end(k, side) == es]
                    for k in places:
                        own_side(em + 1, side, z == k, lambda c: c.start())

    def ready(m, s):
        if s == 0:
            copies[1 + m].wait()
        elif streamed:
            for q in range(PIECES):
                across(m, order(s), 1 - y, q).wait_recv()

    def weight(m, s):
        return wg[m, pl.ds(pl.multiple_of(order(s) * block, block), block), :]

    def p_copy(l, s):
        return remote(psend.at[l, s], precv.at[l, s], p_send_s.at[l, s], p_recv_s.at[l, s], (y, z, sib))

    def x_copies(l, s):
        return [remote(xsend.at[l, s], xrecv.at[k - 1, l, s], x_send_s.at[k - 1, l, s],
                       x_recv_s.at[k - 1, l, s], (y, z, lax.rem(x + k, nx) * 2 + core))
                for k in range(1, nx)]

    def h_copy(l, s):
        b = order(s)
        return remote(hsend.at[l, b], hrecv.at[l, b], h_send_s.at[l, b], h_recv_s.at[l, b],
                      (y, z + core, sib))

    def c_copy(l, s, at):
        ref = sc.at[l, s, pl.ds(at, half)]
        return remote(ref, ref, c_send_s.at[l, s], c_recv_s.at[l, s], (y, z, sib))

    def t_copies(l, i):
        return [remote(tsend.at[l, i], trecv.at[k - 1, l, i], t_send_s.at[k - 1, l, i],
                       t_recv_s.at[k - 1, l, i], (y, z, lax.rem(t + k, tp_n)))
                for k in range(1, tp_n)]

    h_out = (core == 0) | (z < n - 1)
    h_in = (core == 1) | (z > 0)

    def project(l, s):
        w = weight(2 * l, s)
        psend[l, s] = lax.dot_general(
            cur[pl.ds(other, half), :], w, NT, preferred_element_type=F32).astype(BF16)
        p_copy(l, s).start()
        pown[s] = lax.dot_general(cur[pl.ds(mine, half), :], w, NT, preferred_element_type=F32)

    def chip_sum(l, s):
        p_copy(l, s).wait_recv()
        total = pown[s] + precv[l, s].astype(F32)
        pown[s] = total
        xsend[l, s] = total.astype(BF16)
        for copy in x_copies(l, s):
            copy.start()

    def finish_hidden(l, s):
        total = pown[s]
        for k, copy in enumerate(x_copies(l, s)):
            copy.wait_recv()
            total = total + xrecv[k, l, s].astype(F32)
        hidden = total.astype(BF16)
        hbuf[s, REACH:, :] = hidden.astype(F32)
        hsend[l, order(s)] = hidden[half - REACH:, :]
        pl.when(h_out)(h_copy(l, s).start)

    def pool(l, s):
        b = order(s)

        @pl.when(h_in)
        def _():
            h_copy(l, s).wait_recv()
            hbuf[s, :REACH, :] = hrecv[l, b].astype(F32)

        @pl.when(jnp.logical_not(h_in))
        def _():
            hbuf[s, :REACH, :] = jnp.zeros((REACH, width), F32)

        ext = hbuf[s]
        run = ext + pltpu.roll(ext, 1, 0)
        for octave in range(1, groups):
            take = jnp.where(b >= octave, 1.0, 0.0).astype(F32)
            run = run + take * pltpu.roll(run, 2**octave, 0)
        reach = jnp.int32(2)
        for octave in range(1, groups):
            reach = jnp.where(b >= octave, 2 ** (octave + 1), reach)
        at = z * tokens + core * half + 1 + lax.broadcasted_iota(jnp.int32, (half, width), 0)
        counts = jnp.minimum(at, reach).astype(F32)
        pooled = (run[REACH:, :] / counts - ext[REACH:, :]).astype(BF16)
        mixed = jnp.dot(pooled, mix[l, b], preferred_element_type=F32)
        sc[l, s, pl.ds(mine, half), :] = (mixed * gain[l:l + 1, pl.ds(pl.multiple_of(b * width, width), width)]).astype(BF16)
        c_copy(l, s, mine).start()

    def expand(l, s):
        c_copy(l, s, other).wait_recv()
        at_m = 2 * l + 1

        def body(i, carry):
            r = pl.ds(pl.multiple_of(i * block, block), block)
            add = jnp.dot(sc[l, s, r, :], weight(at_m, s), preferred_element_type=F32)
            if s == 0:
                acc[r, :] = alpha * cur[r, :].astype(F32) + add
            else:
                acc[r, :] = acc[r, :] + add
            return carry

        if s < groups - 1:
            lax.fori_loop(0, chunks, body, 0)
            return
        for i in range(chunks):
            body(i, 0)
            v = acc[i * block:(i + 1) * block, :]
            lane = lax.broadcasted_iota(jnp.int32, (block, 128), 1)
            row_sum = jnp.sum(v, axis=1, keepdims=True)
            row_squares = jnp.sum(v * v, axis=1, keepdims=True)
            both = jnp.where(lane == 0, row_sum, jnp.where(lane == 1, row_squares, 0.0))
            tsend[l, i] = both.T[:8, :]
            for copy in t_copies(l, i):
                copy.start()

    def norm(l):
        dst = out if l == layers - 1 else cur
        for i in range(chunks):
            stats = tsend[l, i]
            for k, copy in enumerate(t_copies(l, i)):
                copy.wait_recv()
                stats = stats + trecv[k, l, i]
            stats = stats / d_model
            mean = stats[0:1, :]
            var = stats[1:2, :] - mean * mean
            inv = lax.rsqrt(var + EPSILON)
            row = lax.broadcasted_iota(jnp.int32, (128, block), 0)
            cols = jnp.where(row == 0, mean, jnp.where(row == 1, inv, 0.0)).T
            r = slice(i * block, (i + 1) * block)
            v = (acc[r, :] - cols[:, 0:1]) * cols[:, 1:2]
            dst[r, :] = (v * norm_gain[l:l + 1, :] + norm_shift[l:l + 1, :]).astype(BF16)

    if streamed:
        for m in range(2 * layers):
            for side in (1, 0):
                first = (z >= 0) if m == 0 else (z == 0 if side else z == n - 1)
                own_side(m, side, first, lambda c: c.start())
    copies[0].wait()
    last = groups - 1
    for l in range(layers):
        mi, mo = 2 * l, 2 * l + 1
        ready(mi, 0)
        project(l, 0)
        for s in range(1, groups):
            advance(mi, s, 4)
            chip_sum(l, s - 1)
            ready(mi, s)
            project(l, s)
        chip_sum(l, last)
        for s in range(groups):
            finish_hidden(l, s)
        pool(l, 0)
        pool(l, 1)
        advance(mo, 2)
        for s in range(2, groups):
            pool(l, s)
        ready(mo, 0)
        expand(l, 0)
        for s in range(1, groups):
            advance(mo, s, 4)
            ready(mo, s)
            expand(l, s)
        norm(l)

    if streamed:
        for m in range(2 * layers):
            for side in (1, 0):
                own_side(m, side, z >= 0, lambda c: c.wait_send())
            for s in range(1, n):
                b = order(s)
                for q in range(PIECES):
                    there, copy = onward(m, b, q)
                    pl.when(there)(copy.wait_send)
                    across(m, b, y, q).wait_send()
    for l in range(layers):
        for s in range(groups):
            p_copy(l, s).wait_send()
            for copy in x_copies(l, s):
                copy.wait_send()
            pl.when(h_out)(h_copy(l, s).wait_send)
            c_copy(l, s, mine).wait_send()
        for i in range(chunks):
            for copy in t_copies(l, i):
                copy.wait_send()


def per_device(n, grp_n, tp_n, stream, in_weight, out_weight, group_mix, pool_gain, norm_gain, norm_shift):
    layers, groups, width = group_mix.shape[:3]
    tokens, chans = stream.shape
    pool = groups * width
    streamed = n == groups and grp_n == 2
    if not streamed:
        in_weight = lax.all_gather(in_weight, "sp", axis=1, tiled=True)
        out_weight = lax.all_gather(out_weight, "sp", axis=1, tiled=True)
    nx = tp_n // 2
    half = tokens // 2
    chunks = tokens // 256
    ms = 2 * layers
    dma = pltpu.SemaphoreType.DMA
    any_spec = pl.BlockSpec(memory_space=pl.ANY)
    vmem = pl.BlockSpec(memory_space=pltpu.VMEM)
    xs = max(nx - 1, 1)
    return pl.pallas_call(
        functools.partial(kernel, (n, tp_n, layers, groups, width, streamed)),
        out_shape=jax.ShapeDtypeStruct((tokens, chans), BF16),
        in_specs=[any_spec] * 3 + [vmem] * 4,
        out_specs=vmem,
        scratch_shapes=[
            pltpu.VMEM((ms, pool, chans), BF16),
            pltpu.VMEM((tokens, chans), BF16),
            pltpu.VMEM((tokens, chans), F32),
            pltpu.VMEM((layers, groups, half, width), BF16),
            pltpu.VMEM((layers, groups, half, width), BF16),
            pltpu.VMEM((groups, half, width), F32),
            pltpu.VMEM((layers, groups, half, width), BF16),
            pltpu.VMEM((xs, layers, groups, half, width), BF16),
            pltpu.VMEM((groups, REACH + half, width), F32),
            pltpu.VMEM((layers, groups, REACH, width), BF16),
            pltpu.VMEM((layers, groups, REACH, width), BF16),
            pltpu.VMEM((layers, groups, tokens, width), BF16),
            pltpu.VMEM((layers, chunks, 8, 256), F32),
            pltpu.VMEM((tp_n - 1, layers, chunks, 8, 256), F32),
            dma((1 + ms,)),
            dma((ms, 2, PIECES)), dma((ms, groups, PIECES)), dma((ms, groups, PIECES)),
            dma((ms, groups, PIECES)), dma((ms, groups, PIECES)),
            dma((layers, groups)), dma((layers, groups)),
            dma((xs, layers, groups)), dma((xs, layers, groups)),
            dma((layers, groups)), dma((layers, groups)),
            dma((layers, groups)), dma((layers, groups)),
            dma((tp_n - 1, layers, chunks)), dma((tp_n - 1, layers, chunks)),
            dma((1,)),
        ],
        compiler_params=pltpu.CompilerParams(
            collective_id=0, has_side_effects=True, vmem_limit_bytes=56 * 1024 * 1024),
    )(stream, in_weight, out_weight, group_mix,
      pool_gain, norm_gain, norm_shift)


def solution(mesh):
    in_specs = (
        P(("grp", "sp"), "tp"),
        P(None, "sp", "tp"),
        P(None, "sp", "tp"),
        P(),
        P(),
        P(None, "tp"),
        P(None, "tp"),
    )
    out_specs = P(("grp", "sp"), "tp")
    sizes = mesh.shape
    body = functools.partial(per_device, sizes["sp"], sizes["grp"], sizes["tp"])
    return jax.shard_map(
        body, mesh=mesh, in_specs=in_specs, out_specs=out_specs, check_vma=False
    )
```
